32 devices in a mesh: ep: 32 (over z, y, x, core).
Axes of the slice: x: 2, y: 2, z: 4, core: 2. Of those that a mesh axis runs over, the one named last changes fastest.
Arguments:
- tokens: bfloat16 [4096, 2048], P('ep'), may hold values from -6 to 6
- norm_gain: float32 [2048], replicated, may hold values from 0.1 to 1.9
- expert_ids: int32 [4096, 4], P('ep'), may hold values from 0 to 63, as said below
- gate_weights: float32 [4096, 4], P('ep'), may hold values from 0.1 to 0.6
- expert_gate: bfloat16 [64, 2048, 512], P('ep'), may hold values from -0.125 to 0.125
- expert_up: bfloat16 [64, 2048, 512], P('ep'), may hold values from -0.125 to 0.125
- expert_down: bfloat16 [64, 512, 2048], P('ep'), may hold values from -0.25 to 0.25
- shared_gate: bfloat16 [2048, 512], P('ep'), may hold values from -0.125 to 0.125
- shared_up: bfloat16 [2048, 512], P('ep'), may hold values from -0.125 to 0.125
- shared_down: bfloat16 [512, 2048], P(None, 'ep'), may hold values from -0.25 to 0.25
Outputs:
- mixed: bfloat16 [4096, 2048], P('ep')
The draws below stay inside these ranges and needn't reach their ends.
Inputs may be any that keep to these rules, and one draw needn't show every extreme that they name: `expert_ids`: expert e belongs to device e // 2; each row names 4 experts of 4 different devices; among the rows of one device at most 24 name experts of any one device, hence at most 24 any one expert; in every aligned block of 128 rows exactly 24 rows name one and the same expert.
All inputs are finite; a program needn't handle non-finite values.
Results may differ from the reference program's by a relative error of at most 0.0067.
Values may be sent and summed in bfloat16 or wider, within the bound.
No kernel may reach another device: no remote copies, remote signals or barrier semaphores. Data moves between devices by JAX's collectives and lax.ppermute only.
A program may use at most 128 MiB of HBM per device.

```python
import jax
import jax.numpy as jnp
from jax import lax

D = 2048
DE = 512
DS = 512
TOP_K = 4
EXP_DEV = 2
TOK_DEV = 128
EXPERTS = 64
TOKENS = 4096


def route_block(block_key):
    holders = EXPERTS // EXP_DEV
    total = TOK_DEV * TOP_K
    mean_rows = total // holders
    extra = mean_rows // 2
    key_order, key_moved, key_bits, key_rows = jax.random.split(block_key, 4)
    order = jax.random.permutation(key_order, holders).astype(jnp.int32)
    moved = jax.random.randint(key_moved, (holders // 2,), 0, extra + 1).astype(jnp.int32)
    moved = moved.at[0].set(extra)
    counts = jnp.full((holders,), mean_rows, jnp.int32)
    counts = counts.at[order[0::2]].add(moved).at[order[1::2]].add(-moved)
    ends = jnp.cumsum(counts).astype(jnp.int32)
    slots = jnp.arange(total, dtype=jnp.int32)
    slot_dev = jnp.sum((ends[None, :] <= slots[:, None]).astype(jnp.int32), axis=1).astype(jnp.int32)
    bits = jax.random.randint(key_bits, (total,), 0, EXP_DEV).astype(jnp.int32)
    bits = jnp.where(slot_dev == order[0], 0, bits).astype(jnp.int32)
    expert = (slot_dev * EXP_DEV + bits).astype(jnp.int32)
    row_perm = jax.random.permutation(key_rows, TOK_DEV).astype(jnp.int32)
    row_of = row_perm[slots % TOK_DEV]
    column = (slots // TOK_DEV).astype(jnp.int32)
    table = jnp.zeros((TOK_DEV, TOP_K), jnp.int32).at[row_of, column].set(expert)
    return table


def draw_expert_ids(key, part):
    base = jax.random.fold_in(key, 7117)
    keys = jax.random.split(base, TOKENS // TOK_DEV)
    tables = jax.vmap(route_block)(keys)
    return tables.reshape(TOKENS, TOP_K).astype(jnp.int32)


def levels(key, extent, cuts, low, high):
    gain = 1.0
    for dim, blocks in cuts:
        steps = jax.random.uniform(jax.random.fold_in(jax.random.fold_in(key, 6), dim), (blocks,), jnp.float32, low / len(cuts), high / len(cuts))
        gain = gain * jnp.repeat(jnp.exp(steps), extent[dim] // blocks).reshape((-1,) + (1,) * (len(extent) - 1 - dim))
    return gain


def bell_draw(own_key, dims, scale, bound, shards=(), held_as=jnp.bfloat16):
    result = scale * jax.random.normal(own_key, dims, jnp.float32)
    if shards:
        result = result * levels(own_key, dims, shards, -0.22, 0.18)
    return jnp.clip(result, -bound, bound).astype(held_as)


def setup_inputs(seed: int = 0) -> dict:
    splits = jax.random.split(jax.random.key(seed), 11)
    return {
        "tokens": bell_draw(splits[0], (TOKENS, D), 1.0, 6.0, ((0, 32),)),
        "norm_gain": jnp.clip(1.0 + 0.18 * jax.random.normal(splits[1], (D,), jnp.float32), 0.1, 1.9),
        "expert_ids": draw_expert_ids(jax.random.fold_in(splits[10], 71), 0),
        "gate_weights": jnp.clip(0.1 + 0.5 * jax.random.uniform(splits[3], (TOKENS, TOP_K), jnp.float32) ** levels(splits[3], (TOKENS, TOP_K), ((0, 32),), -0.2, 0.2), 0.1, 0.6),
        "expert_gate": bell_draw(splits[4], (EXPERTS, D, DE), D ** -0.5, 0.125, ((0, 32),)),
        "expert_up": bell_draw(splits[5], (EXPERTS, D, DE), D ** -0.5, 0.125, ((0, 32),)),
        "expert_down": bell_draw(splits[6], (EXPERTS, DE, D), DE ** -0.5, 0.25, ((0, 32),)),
        "shared_gate": bell_draw(splits[7], (D, DS), D ** -0.5, 0.125, ((0, 32),)),
        "shared_up": bell_draw(splits[8], (D, DS), D ** -0.5, 0.125, ((0, 32),)),
        "shared_down": bell_draw(splits[9], (DS, D), DS ** -0.5, 0.25, ((1, 32),)),
    }


EPS = 1e-06

def normalize(tokens, norm_gain):
    values = tokens.astype(jnp.float32)
    scaled = values * lax.rsqrt(lax.optimization_barrier(jnp.mean(values * values, axis=-1, keepdims=True)) + EPS)
    return (scaled * norm_gain.astype(jnp.float32)).astype(jnp.bfloat16)

def swiglu(inputs, w_gate, w_up, w_down):
    gate_val = jnp.dot(inputs, w_gate, preferred_element_type=jnp.float32)
    up_val = jnp.dot(inputs, w_up, preferred_element_type=jnp.float32)
    hidden = (jax.nn.silu(gate_val) * up_val).astype(jnp.bfloat16)
    return jnp.dot(hidden, w_down, preferred_element_type=jnp.float32)

def reference(tokens, norm_gain, expert_ids, gate_weights, expert_gate, expert_up, expert_down, shared_gate, shared_up, shared_down):
    normed = normalize(tokens, norm_gain)
    count_tok = normed.shape[0]
    width = normed.shape[1]
    assign = count_tok * TOP_K
    flat_ids = expert_ids.reshape(assign).astype(jnp.int32)
    ordering = jnp.argsort(flat_ids, stable=True).astype(jnp.int32)
    sorted_ids = flat_ids[ordering]
    sorted_tok = (ordering // TOP_K).astype(jnp.int32)
    sorted_wts = gate_weights.reshape(assign)[ordering]
    counts = jnp.bincount(flat_ids, length=EXPERTS).astype(jnp.int32)
    block_rows = 256
    padded = ((counts + block_rows - 1) // block_rows * block_rows).astype(jnp.int32)
    pad_end = jnp.cumsum(padded).astype(jnp.int32)
    pad_start = pad_end - padded
    cnt_start = (jnp.cumsum(counts).astype(jnp.int32) - counts).astype(jnp.int32)
    dest = (pad_start[sorted_ids] + jnp.arange(assign, dtype=jnp.int32) - cnt_start[sorted_ids]).astype(jnp.int32)
    blocks = -(-(assign + EXPERTS * (block_rows - 1)) // block_rows)
    total_rows = blocks * block_rows
    row_tok = jnp.full((total_rows,), count_tok, jnp.int32).at[dest].set(sorted_tok)
    row_wts = jnp.zeros((total_rows,), jnp.float32).at[dest].set(sorted_wts)
    block_expert = jnp.minimum(jnp.searchsorted(pad_end, jnp.arange(blocks, dtype=jnp.int32) * block_rows, side='right'), EXPERTS - 1).astype(jnp.int32)
    padded_x = jnp.concatenate([normed, jnp.zeros((1, width), jnp.bfloat16)], axis=0)

    def step(accum, inputs_blk):
        tok_blk, wts_blk, expert = inputs_blk
        picked = padded_x[tok_blk]
        output = swiglu(picked, expert_gate[expert], expert_up[expert], expert_down[expert]).astype(jnp.bfloat16)
        accum = accum.at[tok_blk].add(output.astype(jnp.float32) * wts_blk[:, None])
        return (accum, None)
    routed, _ = lax.scan(step, jnp.zeros((count_tok + 1, width), jnp.float32), (row_tok.reshape(blocks, block_rows), row_wts.reshape(blocks, block_rows), block_expert))
    shared = swiglu(normed, shared_gate, shared_up, shared_down)
    return (routed[:count_tok] + shared).astype(jnp.bfloat16)
```

```python
import functools

import jax
import jax.numpy as jnp
from jax import lax
from jax.experimental import pallas as pl
from jax.experimental.pallas import tpu as pltpu
from jax.sharding import PartitionSpec as P


EPS = 1e-06
LANES = 128
F32 = jnp.float32
BF16 = jnp.bfloat16


VMEM = pl.BlockSpec(memory_space=pltpu.VMEM)
SMEM = pl.BlockSpec(memory_space=pltpu.SMEM)


def routes(place_ref, ids_ref, weights_ref, local_experts, slots, cap):
    top, count = ids_ref.shape
    rows = slots * cap
    ids = ids_ref[...]
    weights = weights_ref[...]
    target = ids // local_experts
    local = (ids % local_experts).astype(F32)
    device = place_ref[0] + (
        lax.broadcasted_iota(jnp.int32, (slots, count), 0) ^ place_ref[1]
    )
    zero = jnp.zeros((slots, count), F32)
    member, weight, label = zero, zero, zero
    for k in range(top):
        hit = target[k : k + 1, :] == device
        member = jnp.where(hit, 1.0, member)
        weight = jnp.where(hit, weights[k : k + 1, :], weight)
        label = jnp.where(hit, local[k : k + 1, :], label)
    square = lambda dim: lax.broadcasted_iota(jnp.int32, (count, count), dim)
    before = (square(0) < square(1)).astype(BF16)
    rank = jnp.dot(member.astype(BF16), before, preferred_element_type=F32)
    rank = jnp.where(member > 0.0, rank, -1.0)
    row = lax.broadcasted_iota(jnp.int32, (rows, slots), 0)
    expand = (row // cap == lax.broadcasted_iota(jnp.int32, (rows, slots), 1)).astype(BF16)
    spread = lambda array: jnp.dot(expand, array.astype(BF16), preferred_element_type=F32)
    want = (lax.broadcasted_iota(jnp.int32, (rows, count), 0) % cap).astype(F32)
    pick = (spread(rank) == want).astype(F32)
    labels = jnp.sum(pick * spread(label), axis=1, keepdims=True)
    labels = jnp.broadcast_to(labels, (rows, LANES)).astype(BF16)
    high = weight.astype(BF16).astype(F32)
    mix = jnp.concatenate([(pick * spread(high)).T, (pick * spread(weight - high)).T], axis=0)
    return pick.astype(BF16), labels, mix.astype(BF16)


def norm_kernel(tokens_ref, gain_ref, out_ref):
    values = tokens_ref[...].astype(F32)
    scale = lax.rsqrt(jnp.mean(values * values, axis=-1, keepdims=True) + EPS)
    out_ref[...] = (values * scale * gain_ref[...]).astype(BF16)


def front_kernel(place_ref, ids_ref, weights_ref, x_ref, mix_ref, *out_refs, **sizes):
    pick, labels, mix = routes(place_ref, ids_ref, weights_ref, **sizes)
    mix_ref[...] = mix
    width = x_ref.shape[1]
    cap = sizes["cap"]
    sent = jnp.dot(pick, x_ref[...], preferred_element_type=F32).astype(BF16)
    for slot, out_ref in enumerate(out_refs):
        out_ref[:, :width] = sent[slot * cap : (slot + 1) * cap]
        out_ref[:, width:] = labels[slot * cap : (slot + 1) * cap]


def route_kernel(place_ref, ids_ref, weights_ref, pick_ref, label_ref, mix_ref, **sizes):
    pick_ref[...], label_ref[...], mix_ref[...] = routes(
        place_ref, ids_ref, weights_ref, **sizes
    )


def gather_kernel(pick_ref, label_ref, x_ref, out_ref):
    width = x_ref.shape[1]
    out_ref[:, :width] = jnp.dot(pick_ref[...], x_ref[...], preferred_element_type=F32).astype(
        BF16
    )
    out_ref[:, width:] = label_ref[...]


def join(refs, rows_ref):
    start = 0
    for ref in refs:
        rows_ref[start : start + ref.shape[0], :] = ref[...]
        start += ref.shape[0]


def combined(mix_ref, back_ref):
    both = jnp.dot(mix_ref[...], back_ref[...], preferred_element_type=F32)
    count = both.shape[0] // 2
    return both[:count] + both[count:]


def combine_kernel(mix_ref, back_ref, shared_ref, out_ref):
    out_ref[...] = (combined(mix_ref, back_ref) + shared_ref[...]).astype(BF16)


def own_kernel(mix_ref, shared_ref, *refs):
    *back_refs, out_ref, rows_ref = refs
    join(back_refs, rows_ref)
    out_ref[...] = combined(mix_ref, rows_ref) + shared_ref[...]


def add_kernel(own_ref, other_ref, out_ref):
    out_ref[...] = (own_ref[...] + other_ref[...].astype(F32)).astype(BF16)


def expert_kernel(gate_ref, up_ref, down_ref, *refs, pieces, cuts, outs):
    in_refs, out_refs = refs[:pieces], refs[pieces : 2 * pieces]
    gate_buf, up_buf, down_buf, hidden_ref, sems, *rest = refs[2 * pieces :]
    rows_ref = rest[0] if rest else in_refs[0]
    experts, width, hidden = gate_ref.shape
    block = hidden // cuts
    parts = [(e, pl.ds(j * block, block)) for e in range(experts) for j in range(cuts)]
    firsts = []
    for i, (e, cols) in enumerate(parts):
        pair = [
            pltpu.make_async_copy(src.at[e, :, cols], dst.at[i], sems.at[k, i])
            for k, (src, dst) in enumerate(((gate_ref, gate_buf), (up_ref, up_buf)))
        ]
        for copy in pair:
            copy.start()
        firsts.append(pair)
    piece = width // outs
    seconds = []
    for i in range(outs):
        cols = pl.ds(i * piece, piece)
        copy = pltpu.make_async_copy(down_ref.at[:, cols], down_buf.at[i], sems.at[2, i])
        copy.start()
        seconds.append(copy)
    if rest:
        join(in_refs, rows_ref)
    for i, (e, _) in enumerate(parts):
        for copy in firsts[i]:
            copy.wait()
        rows = rows_ref[:, :width]
        mine = rows_ref[:, width:][:, :1].astype(F32) == float(e)
        gate_val = jnp.dot(rows, gate_buf[i], preferred_element_type=F32)
        up_val = jnp.dot(rows, up_buf[i], preferred_element_type=F32)
        value = jnp.where(mine, gate_val / (1.0 + jnp.exp(-gate_val)) * up_val, 0.0)
        hidden_ref[:, i * block : (i + 1) * block] = value.astype(BF16)
    for i, copy in enumerate(seconds):
        copy.wait()
        result = jnp.dot(
            hidden_ref[...], down_buf[i], preferred_element_type=F32
        ).astype(BF16)
        start = 0
        for out_ref in out_refs:
            stop = start + out_ref.shape[0]
            out_ref[:, i * piece : (i + 1) * piece] = result[start:stop]
            start = stop


def run_experts(rows, w_gate, w_up, w_down):
    experts, width, hidden = w_gate.shape
    cuts, outs = 2, 2
    steps = experts * cuts
    block, piece = hidden // cuts, width // outs
    count = sum(part.shape[0] for part in rows)
    scratch = [
        pltpu.VMEM((steps, width, block), BF16),
        pltpu.VMEM((steps, width, block), BF16),
        pltpu.VMEM((outs, experts * hidden, piece), BF16),
        pltpu.VMEM((count, experts * hidden), BF16),
        pltpu.SemaphoreType.DMA((3, max(steps, outs))),
    ]
    if len(rows) > 1:
        scratch.append(pltpu.VMEM((count, rows[0].shape[1]), BF16))
    return pl.pallas_call(
        functools.partial(expert_kernel, pieces=len(rows), cuts=cuts, outs=outs),
        in_specs=[pl.BlockSpec(memory_space=pltpu.HBM)] * 3 + [VMEM] * len(rows),
        out_specs=[VMEM] * len(rows),
        out_shape=[jax.ShapeDtypeStruct((part.shape[0], width), BF16) for part in rows],
        scratch_shapes=scratch,
        cost_estimate=pl.CostEstimate(
            flops=6 * count * experts * width * hidden,
            bytes_accessed=6 * experts * width * hidden + 4 * count * width,
            transcendentals=count * experts * hidden,
        ),
        compiler_params=pltpu.CompilerParams(vmem_limit_bytes=60 << 20),
    )(w_gate, w_up, w_down.reshape(experts * hidden, width), *rows)


def shared_kernel(me_ref, parts_ref, own_ref, other_ref, out_own_ref, out_other_ref,
                  gate_ref, up_ref, down_ref, *, offsets):
    me = me_ref[0]
    block = parts_ref.shape[2]
    for place, offset in enumerate(offsets):
        start = pl.multiple_of((me ^ offset) * block, block)
        gate_ref[pl.ds(start, block), :] = parts_ref[place, 0]
        up_ref[pl.ds(start, block), :] = parts_ref[place, 1]
        down_ref[pl.ds(start, block), :] = parts_ref[place, 2]
    for x_ref, out_ref in ((own_ref, out_own_ref), (other_ref, out_other_ref)):
        x = x_ref[...]
        gate_val = jnp.dot(x, gate_ref[...], preferred_element_type=F32)
        up_val = jnp.dot(x, up_ref[...], preferred_element_type=F32)
        hidden = (gate_val / (1.0 + jnp.exp(-gate_val)) * up_val).astype(BF16)
        out_ref[...] = lax.dot_general(
            hidden, down_ref[...], (((1,), (1,)), ((), ())), preferred_element_type=F32
        )


def call(kernel, out, args, scalars=1, flops=0, vmem=24, **options):
    shapes = jax.tree.leaves(out)
    specs = jax.tree.map(lambda _: VMEM, out)
    return pl.pallas_call(
        kernel,
        in_specs=[SMEM] * scalars + [VMEM] * (len(args) - scalars),
        out_specs=specs,
        out_shape=out,
        cost_estimate=pl.CostEstimate(
            flops=flops,
            bytes_accessed=sum(a.size * a.dtype.itemsize for a in list(args) + shapes),
            transcendentals=0,
        ),
        compiler_params=pltpu.CompilerParams(vmem_limit_bytes=vmem << 20),
        **options,
    )(*args)


def per_device(
    tokens,
    norm_gain,
    expert_ids,
    gate_weights,
    expert_gate,
    expert_up,
    expert_down,
    shared_gate,
    shared_up,
    shared_down,
):
    devices = lax.axis_size("ep")
    me = lax.axis_index("ep").astype(jnp.int32)
    half = devices // 2
    side = me // half
    count, top = expert_ids.shape
    width = tokens.shape[1]
    mean_rows = count * top // devices
    cap = -(-(mean_rows + mean_rows // 2) // 8) * 8
    rows = half * cap
    sizes = dict(local_experts=expert_gate.shape[0], slots=half, cap=cap)
    groups = [list(range(half)), list(range(half, devices))]

    def exchange(array, bit):
        return lax.ppermute(array, "ep", [(i, i ^ bit) for i in range(devices)])

    def within(array):
        return lax.all_to_all(array, "ep", 0, 0, axis_index_groups=groups, tiled=True)

    base = side * half
    place = jnp.stack([base, me % half])
    place_other = jnp.stack([base, jnp.zeros_like(me)])
    dense = jax.ShapeDtypeStruct((count, width), BF16)
    plan = (
        jax.ShapeDtypeStruct((rows, count), BF16),
        jax.ShapeDtypeStruct((rows, LANES), BF16),
        jax.ShapeDtypeStruct((2 * count, rows), BF16),
    )
    sent = jax.ShapeDtypeStruct((rows, width + LANES), BF16)
    work = 2 * rows * count * width
    few = 8 * rows * count * half

    parts = jnp.stack([shared_gate, shared_up, shared_down.T])[None]
    cut = parts.shape[3] // 2
    offsets = [0]
    for bit in shared_steps(devices):
        if bit == half:
            low, high = parts[..., :cut], parts[..., cut:]
            mine = jnp.where(side == 0, low, high)
            theirs = jnp.where(side == 0, high, low)
        else:
            mine = theirs = parts
        parts = jnp.concatenate([mine, exchange(theirs, bit)], axis=0)
        offsets += [offset ^ bit for offset in offsets]

    ids, weights = expert_ids.T, gate_weights.T
    ids_other = exchange(ids, half)
    weights_other = exchange(weights, half)
    piece = jax.ShapeDtypeStruct((cap, width + LANES), BF16)
    normed = call(
        norm_kernel, dense, (tokens, norm_gain.reshape(1, width)),
        scalars=0, flops=8 * count * width,
    )
    normed_other = exchange(normed, half)
    mix, *outgoing = call(
        functools.partial(front_kernel, **sizes), [plan[2]] + [piece] * half,
        (place, ids, weights, normed), flops=work + few,
    )
    incoming = [outgoing[0]] + [exchange(outgoing[r], r) for r in range(1, half)]
    pick, label, mix_other = call(
        functools.partial(route_kernel, **sizes), plan,
        (place_other, ids_other, weights_other), flops=few,
    )
    outgoing_other = call(gather_kernel, sent, (pick, label, normed_other), scalars=0, flops=work)
    incoming_other = within(outgoing_other)
    results = run_experts(incoming, expert_gate, expert_up, expert_down)
    (results_other,) = run_experts([incoming_other], expert_gate, expert_up, expert_down)
    back_other = within(results_other)
    back = [results[0]] + [exchange(results[r], r) for r in range(1, half)]

    block = shared_gate.shape[0]
    full = pltpu.VMEM((devices * block, cut), BF16)
    shape = jax.ShapeDtypeStruct((count, width), F32)
    shared_own, shared_other = call(
        functools.partial(shared_kernel, offsets=tuple(offsets)),
        (shape, shape),
        (me.reshape(1), parts, normed, normed_other),
        flops=12 * count * width * cut,
        scratch_shapes=[full, full, full],
    )
    partial = call(
        combine_kernel, dense, (mix_other, back_other, shared_other),
        scalars=0, flops=2 * work,
    )
    from_other = exchange(partial, half)
    total = call(
        own_kernel, shape, (mix, shared_own, *back),
        scalars=0, flops=2 * work, scratch_shapes=[pltpu.VMEM((rows, width), BF16)],
    )
    return call(add_kernel, dense, (total, from_other), scalars=0, flops=count * width)


def shared_steps(devices):
    half = devices // 2
    bits = [1 << b for b in range(devices.bit_length() - 3, -1, -1)]
    early = [bit for bit in bits if 2 <= bit <= 4]
    late = [bit for bit in bits if 4 < bit]
    return early + [half] + late + [1]


def solution(mesh):
    return jax.shard_map(
        per_device,
        mesh=mesh,
        in_specs=(
            P("ep", None),
            P(),
            P("ep", None),
            P("ep", None),
            P("ep", None, None),
            P("ep", None, None),
            P("ep", None, None),
            P("ep", None),
            P("ep", None),
            P(None, "ep"),
        ),
        out_specs=P("ep", None),
        check_vma=False,
    )
```

```python
import functools

import jax
import jax.numpy as jnp
from jax import lax
from jax.experimental import pallas as pl
from jax.experimental.pallas import tpu as pltpu
from jax.sharding import PartitionSpec as P


EPS = 1e-06
LANES = 128
F32 = jnp.float32
BF16 = jnp.bfloat16


VMEM = pl.BlockSpec(memory_space=pltpu.VMEM)
SMEM = pl.BlockSpec(memory_space=pltpu.SMEM)


def routes(place_ref, ids_ref, weights_ref, local_experts, slots, cap):
    top, count = ids_ref.shape
    rows = slots * cap
    ids = ids_ref[...]
    weights = weights_ref[...]
    target = ids // local_experts
    local = (ids % local_experts).astype(F32)
    device = place_ref[0] + (
        lax.broadcasted_iota(jnp.int32, (slots, count), 0) ^ place_ref[1]
    )
    zero = jnp.zeros((slots, count), F32)
    member, weight, label = zero, zero, zero
    for k in range(top):
        hit = target[k : k + 1, :] == device
        member = jnp.where(hit, 1.0, member)
        weight = jnp.where(hit, weights[k : k + 1, :], weight)
        label = jnp.where(hit, local[k : k + 1, :], label)
    square = lambda dim: lax.broadcasted_iota(jnp.int32, (count, count), dim)
    before = (square(0) < square(1)).astype(BF16)
    rank = jnp.dot(member.astype(BF16), before, preferred_element_type=F32)
    rank = jnp.where(member > 0.0, rank, -1.0)
    row = lax.broadcasted_iota(jnp.int32, (rows, slots), 0)
    expand = (row // cap == lax.broadcasted_iota(jnp.int32, (rows, slots), 1)).astype(BF16)
    spread = lambda array: jnp.dot(expand, array.astype(BF16), preferred_element_type=F32)
    want = (lax.broadcasted_iota(jnp.int32, (rows, count), 0) % cap).astype(F32)
    pick = (spread(rank) == want).astype(F32)
    labels = jnp.sum(pick * spread(label), axis=1, keepdims=True)
    labels = jnp.broadcast_to(labels, (rows, LANES)).astype(BF16)
    high = weight.astype(BF16).astype(F32)
    mix = jnp.concatenate([(pick * spread(high)).T, (pick * spread(weight - high)).T], axis=0)
    return pick.astype(BF16), labels, mix.astype(BF16)


def norm_kernel(tokens_ref, gain_ref, out_ref):
    values = tokens_ref[...].astype(F32)
    scale = lax.rsqrt(jnp.mean(values * values, axis=-1, keepdims=True) + EPS)
    out_ref[...] = (values * scale * gain_ref[...]).astype(BF16)


def front_kernel(place_ref, ids_ref, weights_ref, x_ref, mix_ref, *out_refs, **sizes):
    pick, labels, mix = routes(place_ref, ids_ref, weights_ref, **sizes)
    mix_ref[...] = mix
    width = x_ref.shape[1]
    sent = jnp.dot(pick, x_ref[...], preferred_element_type=F32).astype(BF16)
    start = 0
    for out_ref in out_refs:
        stop = start + out_ref.shape[0]
        out_ref[:, :width] = sent[start:stop]
        out_ref[:, width:] = labels[start:stop]
        start = stop


def route_kernel(place_ref, ids_ref, weights_ref, pick_ref, label_ref, mix_ref, **sizes):
    pick_ref[...], label_ref[...], mix_ref[...] = routes(
        place_ref, ids_ref, weights_ref, **sizes
    )


def gather_kernel(pick_ref, label_ref, x_ref, out_ref):
    width = x_ref.shape[1]
    out_ref[:, :width] = jnp.dot(pick_ref[...], x_ref[...], preferred_element_type=F32).astype(
        BF16
    )
    out_ref[:, width:] = label_ref[...]


def join(refs, rows_ref, takes=None):
    start = 0
    for ref, take in zip(refs, takes or [ref.shape[0] for ref in refs]):
        rows_ref[start : start + take, :] = ref[:take]
        start += take


def swap_kernel(*refs):
    *in_refs, out_ref = refs
    cap = in_refs[0].shape[0] // 2
    for i, ref in enumerate(in_refs):
        out_ref[i * cap : (i + 1) * cap, :] = ref[cap:]


def merge_kernel(kept_ref, swapped_ref, *out_refs):
    cap = out_refs[0].shape[0] // 2
    for i, ref in enumerate(out_refs):
        ref[:cap] = kept_ref[i * cap : (i + 1) * cap, :]
        ref[cap:] = swapped_ref[i * cap : (i + 1) * cap, :]


def combined(mix_ref, back_ref):
    both = jnp.dot(mix_ref[...], back_ref[...], preferred_element_type=F32)
    count = both.shape[0] // 2
    return both[:count] + both[count:]


def combine_kernel(mix_ref, back_ref, shared_ref, out_ref):
    out_ref[...] = (combined(mix_ref, back_ref) + shared_ref[...]).astype(BF16)


def own_kernel(mix_ref, shared_ref, *refs):
    *back_refs, out_ref, rows_ref = refs
    join(back_refs, rows_ref)
    out_ref[...] = combined(mix_ref, rows_ref) + shared_ref[...]


def add_kernel(own_ref, other_ref, out_ref):
    out_ref[...] = (own_ref[...] + other_ref[...].astype(F32)).astype(BF16)


def expert_kernel(gate_ref, up_ref, down_ref, *refs, takes, results, cuts, outs):
    in_refs, out_refs = refs[: len(takes)], refs[len(takes) : len(takes) + results]
    gate_buf, up_buf, down_buf, hidden_ref, sems, *rest = refs[len(takes) + results :]
    rows_ref = rest[0] if rest else in_refs[0]
    experts, width, hidden = gate_ref.shape
    block = hidden // cuts
    parts = [(e, pl.ds(j * block, block)) for e in range(experts) for j in range(cuts)]
    firsts = []
    for i, (e, cols) in enumerate(parts):
        pair = [
            pltpu.make_async_copy(src.at[e, :, cols], dst.at[i], sems.at[k, i])
            for k, (src, dst) in enumerate(((gate_ref, gate_buf), (up_ref, up_buf)))
        ]
        for copy in pair:
            copy.start()
        firsts.append(pair)
    piece = width // outs
    seconds = []
    for i in range(outs):
        cols = pl.ds(i * piece, piece)
        copy = pltpu.make_async_copy(down_ref.at[:, cols], down_buf.at[i], sems.at[2, i])
        copy.start()
        seconds.append(copy)
    if rest:
        join(in_refs, rows_ref, takes)
    for i, (e, _) in enumerate(parts):
        for copy in firsts[i]:
            copy.wait()
        rows = rows_ref[:, :width]
        mine = rows_ref[:, width:][:, :1].astype(F32) == float(e)
        gate_val = jnp.dot(rows, gate_buf[i], preferred_element_type=F32)
        up_val = jnp.dot(rows, up_buf[i], preferred_element_type=F32)
        value = jnp.where(mine, gate_val / (1.0 + jnp.exp(-gate_val)) * up_val, 0.0)
        hidden_ref[:, i * block : (i + 1) * block] = value.astype(BF16)
    for i, copy in enumerate(seconds):
        copy.wait()
        result = jnp.dot(
            hidden_ref[...], down_buf[i], preferred_element_type=F32
        ).astype(BF16)
        start = 0
        for out_ref in out_refs:
            stop = start + out_ref.shape[0]
            out_ref[:, i * piece : (i + 1) * piece] = result[start:stop]
            start = stop


def run_experts(rows, takes, results, w_gate, w_up, w_down):
    experts, width, hidden = w_gate.shape
    cuts, outs = 2, 2
    steps = experts * cuts
    block, piece = hidden // cuts, width // outs
    count = sum(takes)
    scratch = [
        pltpu.VMEM((steps, width, block), BF16),
        pltpu.VMEM((steps, width, block), BF16),
        pltpu.VMEM((outs, experts * hidden, piece), BF16),
        pltpu.VMEM((count, experts * hidden), BF16),
        pltpu.SemaphoreType.DMA((3, max(steps, outs))),
    ]
    if len(rows) > 1:
        scratch.append(pltpu.VMEM((count, rows[0].shape[1]), BF16))
    return pl.pallas_call(
        functools.partial(
            expert_kernel, takes=tuple(takes), results=len(results), cuts=cuts, outs=outs
        ),
        in_specs=[pl.BlockSpec(memory_space=pltpu.HBM)] * 3 + [VMEM] * len(rows),
        out_specs=[VMEM] * len(results),
        out_shape=[jax.ShapeDtypeStruct((part, width), BF16) for part in results],
        scratch_shapes=scratch,
        cost_estimate=pl.CostEstimate(
            flops=6 * count * experts * width * hidden,
            bytes_accessed=6 * experts * width * hidden + 4 * count * width,
            transcendentals=count * experts * hidden,
        ),
        compiler_params=pltpu.CompilerParams(vmem_limit_bytes=60 << 20),
    )(w_gate, w_up, w_down.reshape(experts * hidden, width), *rows)


def shared_kernel(me_ref, parts_ref, own_ref, other_ref, out_own_ref, out_other_ref,
                  gate_ref, up_ref, down_ref, *, offsets):
    me = me_ref[0]
    block = parts_ref.shape[2]
    for place, offset in enumerate(offsets):
        start = pl.multiple_of((me ^ offset) * block, block)
        gate_ref[pl.ds(start, block), :] = parts_ref[place, 0]
        up_ref[pl.ds(start, block), :] = parts_ref[place, 1]
        down_ref[pl.ds(start, block), :] = parts_ref[place, 2]
    for x_ref, out_ref in ((own_ref, out_own_ref), (other_ref, out_other_ref)):
        x = x_ref[...]
        gate_val = jnp.dot(x, gate_ref[...], preferred_element_type=F32)
        up_val = jnp.dot(x, up_ref[...], preferred_element_type=F32)
        hidden = (gate_val / (1.0 + jnp.exp(-gate_val)) * up_val).astype(BF16)
        out_ref[...] = lax.dot_general(
            hidden, down_ref[...], (((1,), (1,)), ((), ())), preferred_element_type=F32
        )


def call(kernel, out, args, scalars=1, flops=0, vmem=24, **options):
    shapes = jax.tree.leaves(out)
    specs = jax.tree.map(lambda _: VMEM, out)
    return pl.pallas_call(
        kernel,
        in_specs=[SMEM] * scalars + [VMEM] * (len(args) - scalars),
        out_specs=specs,
        out_shape=out,
        cost_estimate=pl.CostEstimate(
            flops=flops,
            bytes_accessed=sum(a.size * a.dtype.itemsize for a in list(args) + shapes),
            transcendentals=0,
        ),
        compiler_params=pltpu.CompilerParams(vmem_limit_bytes=vmem << 20),
        **options,
    )(*args)


def per_device(
    tokens,
    norm_gain,
    expert_ids,
    gate_weights,
    expert_gate,
    expert_up,
    expert_down,
    shared_gate,
    shared_up,
    shared_down,
):
    devices = lax.axis_size("ep")
    me = lax.axis_index("ep").astype(jnp.int32)
    half = devices // 2
    side = me // half
    count, top = expert_ids.shape
    width = tokens.shape[1]
    mean_rows = count * top // devices
    cap = -(-(mean_rows + mean_rows // 2) // 8) * 8
    rows = half * cap
    sizes = dict(local_experts=expert_gate.shape[0], slots=half, cap=cap)
    groups = [list(range(half)), list(range(half, devices))]

    def exchange(array, bit):
        return lax.ppermute(array, "ep", [(i, i ^ bit) for i in range(devices)])

    def within(array):
        return lax.all_to_all(array, "ep", 0, 0, axis_index_groups=groups, tiled=True)

    base = side * half
    place = jnp.stack([base, me % half])
    place_other = jnp.stack([base, jnp.zeros_like(me)])
    dense = jax.ShapeDtypeStruct((count, width), BF16)
    plan = (
        jax.ShapeDtypeStruct((rows, count), BF16),
        jax.ShapeDtypeStruct((rows, LANES), BF16),
        jax.ShapeDtypeStruct((2 * count, rows), BF16),
    )
    sent = jax.ShapeDtypeStruct((rows, width + LANES), BF16)
    work = 2 * rows * count * width
    few = 8 * rows * count * half

    parts = jnp.stack([shared_gate, shared_up, shared_down.T])[None]
    cut = parts.shape[3] // 2
    offsets = [0]
    for bit in shared_steps(devices):
        if bit == half:
            low, high = parts[..., :cut], parts[..., cut:]
            mine = jnp.where(side == 0, low, high)
            theirs = jnp.where(side == 0, high, low)
        else:
            mine = theirs = parts
        parts = jnp.concatenate([mine, exchange(theirs, bit)], axis=0)
        offsets += [offset ^ bit for offset in offsets]

    ids, weights = expert_ids.T, gate_weights.T
    ids_other = exchange(ids, half)
    weights_other = exchange(weights, half)
    chips = half // 2
    piece = jax.ShapeDtypeStruct((2 * cap, width + LANES), BF16)
    normed = call(
        norm_kernel, dense, (tokens, norm_gain.reshape(1, width)),
        scalars=0, flops=8 * count * width,
    )
    normed_other = exchange(normed, half)
    mix, *outgoing = call(
        functools.partial(front_kernel, **sizes), [plan[2]] + [piece] * chips,
        (place, ids, weights, normed), flops=work + few,
    )
    incoming = [outgoing[0]] + [exchange(outgoing[m], 2 * m) for m in range(1, chips)]
    crossing = call(
        swap_kernel, jax.ShapeDtypeStruct((rows // 2, width + LANES), BF16), incoming,
        scalars=0,
    )
    crossed = exchange(crossing, 1)
    pick, label, mix_other = call(
        functools.partial(route_kernel, **sizes), plan,
        (place_other, ids_other, weights_other), flops=few,
    )
    outgoing_other = call(gather_kernel, sent, (pick, label, normed_other), scalars=0, flops=work)
    incoming_other = within(outgoing_other)
    experts = (expert_gate, expert_up, expert_down)
    kept, crossing = run_experts(
        incoming + [crossed], [cap] * chips + [rows // 2], [rows // 2] * 2, *experts
    )
    (results_other,) = run_experts([incoming_other], [rows], [rows], *experts)
    back_other = within(results_other)
    crossed = exchange(crossing, 1)
    piece = jax.ShapeDtypeStruct((2 * cap, width), BF16)
    results = call(merge_kernel, [piece] * chips, (kept, crossed), scalars=0)
    back = [results[0]] + [exchange(results[m], 2 * m) for m in range(1, chips)]

    block = shared_gate.shape[0]
    full = pltpu.VMEM((devices * block, cut), BF16)
    shape = jax.ShapeDtypeStruct((count, width), F32)
    shared_own, shared_other = call(
        functools.partial(shared_kernel, offsets=tuple(offsets)),
        (shape, shape),
        (me.reshape(1), parts, normed, normed_other),
        flops=12 * count * width * cut,
        scratch_shapes=[full, full, full],
    )
    partial = call(
        combine_kernel, dense, (mix_other, back_other, shared_other),
        scalars=0, flops=2 * work,
    )
    from_other = exchange(partial, half)
    total = call(
        own_kernel, shape, (mix, shared_own, *back),
        scalars=0, flops=2 * work, scratch_shapes=[pltpu.VMEM((rows, width), BF16)],
    )
    return call(add_kernel, dense, (total, from_other), scalars=0, flops=count * width)


def shared_steps(devices):
    half = devices // 2
    bits = [1 << b for b in range(devices.bit_length() - 3, -1, -1)]
    early = [bit for bit in bits if 2 <= bit <= 4]
    late = [bit for bit in bits if 4 < bit]
    return early + [half] + late + [1]


def solution(mesh):
    return jax.shard_map(
        per_device,
        mesh=mesh,
        in_specs=(
            P("ep", None),
            P(),
            P("ep", None),
            P("ep", None),
            P("ep", None, None),
            P("ep", None, None),
            P("ep", None, None),
            P("ep", None),
            P("ep", None),
            P(None, "ep"),
        ),
        out_specs=P("ep", None),
        check_vma=False,
    )
```

```python
import functools

import jax
import jax.numpy as jnp
from jax import lax
from jax.experimental import pallas as pl
from jax.experimental.pallas import tpu as pltpu
from jax.sharding import PartitionSpec as P


EPS = 1e-06
LANES = 128
F32 = jnp.float32
BF16 = jnp.bfloat16


VMEM = pl.BlockSpec(memory_space=pltpu.VMEM)
SMEM = pl.BlockSpec(memory_space=pltpu.SMEM)


def routes(place_ref, ids_ref, weights_ref, local_experts, slots, cap):
    top, count = ids_ref.shape
    rows = slots * cap
    ids = ids_ref[...]
    weights = weights_ref[...]
    target = ids // local_experts
    local = (ids % local_experts).astype(F32)
    device = place_ref[0] + (
        lax.broadcasted_iota(jnp.int32, (slots, count), 0) ^ place_ref[1]
    )
    zero = jnp.zeros((slots, count), F32)
    member, weight, label = zero, zero, zero
    for k in range(top):
        hit = target[k : k + 1, :] == device
        member = jnp.where(hit, 1.0, member)
        weight = jnp.where(hit, weights[k : k + 1, :], weight)
        label = jnp.where(hit, local[k : k + 1, :], label)
    square = lambda dim: lax.broadcasted_iota(jnp.int32, (count, count), dim)
    before = (square(0) < square(1)).astype(BF16)
    rank = jnp.dot(member.astype(BF16), before, preferred_element_type=F32)
    rank = jnp.where(member > 0.0, rank, -1.0)
    row = lax.broadcasted_iota(jnp.int32, (rows, slots), 0)
    expand = (row // cap == lax.broadcasted_iota(jnp.int32, (rows, slots), 1)).astype(BF16)
    spread = lambda array: jnp.dot(expand, array.astype(BF16), preferred_element_type=F32)
    want = (lax.broadcasted_iota(jnp.int32, (rows, count), 0) % cap).astype(F32)
    pick = (spread(rank) == want).astype(F32)
    labels = jnp.sum(pick * spread(label), axis=1, keepdims=True)
    labels = jnp.broadcast_to(labels, (rows, LANES)).astype(BF16)
    high = weight.astype(BF16).astype(F32)
    mix = jnp.concatenate([(pick * spread(high)).T, (pick * spread(weight - high)).T], axis=0)
    return pick.astype(BF16), labels, mix.astype(BF16)


def norm_kernel(tokens_ref, gain_ref, out_ref):
    values = tokens_ref[...].astype(F32)
    scale = lax.rsqrt(jnp.mean(values * values, axis=-1, keepdims=True) + EPS)
    out_ref[...] = (values * scale * gain_ref[...]).astype(BF16)


def front_kernel(place_ref, ids_ref, weights_ref, x_ref, mix_ref, *out_refs, **sizes):
    pick, labels, mix = routes(place_ref, ids_ref, weights_ref, **sizes)
    mix_ref[...] = mix
    width = x_ref.shape[1]
    sent = jnp.dot(pick, x_ref[...], preferred_element_type=F32).astype(BF16)
    start = 0
    for out_ref in out_refs:
        stop = start + out_ref.shape[0]
        out_ref[:, :width] = sent[start:stop]
        out_ref[:, width:] = labels[start:stop]
        start = stop


def route_kernel(place_ref, ids_ref, weights_ref, pick_ref, label_ref, mix_ref, **sizes):
    pick_ref[...], label_ref[...], mix_ref[...] = routes(
        place_ref, ids_ref, weights_ref, **sizes
    )


def gather_kernel(pick_ref, label_ref, x_ref, out_ref):
    width = x_ref.shape[1]
    out_ref[:, :width] = jnp.dot(pick_ref[...], x_ref[...], preferred_element_type=F32).astype(
        BF16
    )
    out_ref[:, width:] = label_ref[...]


def join(refs, rows_ref, takes=None):
    start = 0
    for ref, take in zip(refs, takes or [ref.shape[0] for ref in refs]):
        rows_ref[start : start + take, :] = ref[:take]
        start += take


def swap_kernel(*refs):
    *in_refs, out_ref = refs
    cap = in_refs[0].shape[0] // 2
    for i, ref in enumerate(in_refs):
        out_ref[i * cap : (i + 1) * cap, :] = ref[cap:]


def merge_kernel(kept_ref, swapped_ref, *out_refs):
    cap = out_refs[0].shape[0] // 2
    for i, ref in enumerate(out_refs):
        ref[:cap] = kept_ref[i * cap : (i + 1) * cap, :]
        ref[cap:] = swapped_ref[i * cap : (i + 1) * cap, :]


def combined(mix_ref, back_ref):
    both = jnp.dot(mix_ref[...], back_ref[...], preferred_element_type=F32)
    count = both.shape[0] // 2
    return both[:count] + both[count:]


def combine_kernel(mix_ref, back_ref, shared_ref, out_ref):
    out_ref[...] = (combined(mix_ref, back_ref) + shared_ref[...]).astype(BF16)


def own_kernel(mix_ref, shared_ref, *refs):
    *back_refs, out_ref, rows_ref = refs
    join(back_refs, rows_ref)
    out_ref[...] = combined(mix_ref, rows_ref) + shared_ref[...]


def add_kernel(own_ref, other_ref, out_ref):
    out_ref[...] = (own_ref[...] + other_ref[...].astype(F32)).astype(BF16)


def expert_kernel(gate_ref, up_ref, down_ref, *refs, takes, results, cuts, outs):
    in_refs, out_refs = refs[: len(takes)], refs[len(takes) : len(takes) + results]
    gate_buf, up_buf, down_buf, hidden_ref, sems, *rest = refs[len(takes) + results :]
    rows_ref = rest[0] if rest else in_refs[0]
    experts, width, hidden = gate_ref.shape
    block = hidden // cuts
    parts = [(e, pl.ds(j * block, block)) for e in range(experts) for j in range(cuts)]
    firsts = []
    for i, (e, cols) in enumerate(parts):
        pair = [
            pltpu.make_async_copy(src.at[e, :, cols], dst.at[i], sems.at[k, i])
            for k, (src, dst) in enumerate(((gate_ref, gate_buf), (up_ref, up_buf)))
        ]
        for copy in pair:
            copy.start()
        firsts.append(pair)
    piece = width // outs
    seconds = []
    for i in range(outs):
        cols = pl.ds(i * piece, piece)
        copy = pltpu.make_async_copy(down_ref.at[:, cols], down_buf.at[i], sems.at[2, i])
        copy.start()
        seconds.append(copy)
    if rest:
        join(in_refs, rows_ref, takes)
    for i, (e, _) in enumerate(parts):
        for copy in firsts[i]:
            copy.wait()
        rows = rows_ref[:, :width]
        mine = rows_ref[:, width:][:, :1].astype(F32) == float(e)
        gate_val = jnp.dot(rows, gate_buf[i], preferred_element_type=F32)
        up_val = jnp.dot(rows, up_buf[i], preferred_element_type=F32)
        value = jnp.where(mine, gate_val / (1.0 + jnp.exp(-gate_val)) * up_val, 0.0)
        hidden_ref[:, i * block : (i + 1) * block] = value.astype(BF16)
    for i, copy in enumerate(seconds):
        copy.wait()
        result = jnp.dot(
            hidden_ref[...], down_buf[i], preferred_element_type=F32
        ).astype(BF16)
        start = 0
        for out_ref in out_refs:
            stop = start + out_ref.shape[0]
            out_ref[:, i * piece : (i + 1) * piece] = result[start:stop]
            start = stop


def run_experts(rows, takes, results, w_gate, w_up, w_down):
    experts, width, hidden = w_gate.shape
    cuts, outs = 2, 2
    steps = experts * cuts
    block, piece = hidden // cuts, width // outs
    count = sum(takes)
    scratch = [
        pltpu.VMEM((steps, width, block), BF16),
        pltpu.VMEM((steps, width, block), BF16),
        pltpu.VMEM((outs, experts * hidden, piece), BF16),
        pltpu.VMEM((count, experts * hidden), BF16),
        pltpu.SemaphoreType.DMA((3, max(steps, outs))),
    ]
    if len(rows) > 1:
        scratch.append(pltpu.VMEM((count, rows[0].shape[1]), BF16))
    return pl.pallas_call(
        functools.partial(
            expert_kernel, takes=tuple(takes), results=len(results), cuts=cuts, outs=outs
        ),
        in_specs=[pl.BlockSpec(memory_space=pltpu.HBM)] * 3 + [VMEM] * len(rows),
        out_specs=[VMEM] * len(results),
        out_shape=[jax.ShapeDtypeStruct((part, width), BF16) for part in results],
        scratch_shapes=scratch,
        cost_estimate=pl.CostEstimate(
            flops=6 * count * experts * width * hidden,
            bytes_accessed=6 * experts * width * hidden + 4 * count * width,
            transcendentals=count * experts * hidden,
        ),
        compiler_params=pltpu.CompilerParams(vmem_limit_bytes=60 << 20),
    )(w_gate, w_up, w_down.reshape(experts * hidden, width), *rows)


def shared_kernel(me_ref, near_ref, far_ref, own_ref, other_ref, out_own_ref, out_other_ref,
                  gate_ref, up_ref, down_ref, *, offsets):
    block = near_ref.shape[2]
    for parts_ref, me in ((near_ref, me_ref[0]), (far_ref, me_ref[0] ^ 1)):
        for place, offset in enumerate(offsets):
            start = pl.multiple_of((me ^ offset) * block, block)
            gate_ref[pl.ds(start, block), :] = parts_ref[place, 0]
            up_ref[pl.ds(start, block), :] = parts_ref[place, 1]
            down_ref[pl.ds(start, block), :] = parts_ref[place, 2]
    for x_ref, out_ref in ((own_ref, out_own_ref), (other_ref, out_other_ref)):
        x = x_ref[...]
        gate_val = jnp.dot(x, gate_ref[...], preferred_element_type=F32)
        up_val = jnp.dot(x, up_ref[...], preferred_element_type=F32)
        hidden = (gate_val / (1.0 + jnp.exp(-gate_val)) * up_val).astype(BF16)
        out_ref[...] = lax.dot_general(
            hidden, down_ref[...], (((1,), (1,)), ((), ())), preferred_element_type=F32
        )


def call(kernel, out, args, scalars=1, flops=0, vmem=24, **options):
    shapes = jax.tree.leaves(out)
    specs = jax.tree.map(lambda _: VMEM, out)
    return pl.pallas_call(
        kernel,
        in_specs=[SMEM] * scalars + [VMEM] * (len(args) - scalars),
        out_specs=specs,
        out_shape=out,
        cost_estimate=pl.CostEstimate(
            flops=flops,
            bytes_accessed=sum(a.size * a.dtype.itemsize for a in list(args) + shapes),
            transcendentals=0,
        ),
        compiler_params=pltpu.CompilerParams(vmem_limit_bytes=vmem << 20),
        **options,
    )(*args)


def per_device(
    tokens,
    norm_gain,
    expert_ids,
    gate_weights,
    expert_gate,
    expert_up,
    expert_down,
    shared_gate,
    shared_up,
    shared_down,
):
    devices = lax.axis_size("ep")
    me = lax.axis_index("ep").astype(jnp.int32)
    half = devices // 2
    side = me // half
    count, top = expert_ids.shape
    width = tokens.shape[1]
    mean_rows = count * top // devices
    cap = -(-(mean_rows + mean_rows // 2) // 8) * 8
    rows = half * cap
    sizes = dict(local_experts=expert_gate.shape[0], slots=half, cap=cap)
    groups = [list(range(half)), list(range(half, devices))]

    def exchange(array, bit):
        return lax.ppermute(array, "ep", [(i, i ^ bit) for i in range(devices)])

    def within(array):
        return lax.all_to_all(array, "ep", 0, 0, axis_index_groups=groups, tiled=True)

    base = side * half
    place = jnp.stack([base, me % half])
    place_other = jnp.stack([base, jnp.zeros_like(me)])
    dense = jax.ShapeDtypeStruct((count, width), BF16)
    plan = (
        jax.ShapeDtypeStruct((rows, count), BF16),
        jax.ShapeDtypeStruct((rows, LANES), BF16),
        jax.ShapeDtypeStruct((2 * count, rows), BF16),
    )
    sent = jax.ShapeDtypeStruct((rows, width + LANES), BF16)
    work = 2 * rows * count * width
    few = 8 * rows * count * half

    parts = jnp.stack([shared_gate, shared_up, shared_down.T])[None]
    cut = parts.shape[3] // 2
    offsets = [0]
    for bit in shared_steps(devices)[:-1]:
        if bit == half:
            low, high = parts[..., :cut], parts[..., cut:]
            mine = jnp.where(side == 0, low, high)
            theirs = jnp.where(side == 0, high, low)
        else:
            mine = theirs = parts
        parts = jnp.concatenate([mine, exchange(theirs, bit)], axis=0)
        offsets += [offset ^ bit for offset in offsets]
    far_parts = exchange(parts, 1)

    ids, weights = expert_ids.T, gate_weights.T
    ids_other = exchange(ids, half)
    weights_other = exchange(weights, half)
    chips = half // 2
    piece = jax.ShapeDtypeStruct((2 * cap, width + LANES), BF16)
    normed = call(
        norm_kernel, dense, (tokens, norm_gain.reshape(1, width)),
        scalars=0, flops=8 * count * width,
    )
    normed_other = exchange(normed, half)
    mix, *outgoing = call(
        functools.partial(front_kernel, **sizes), [plan[2]] + [piece] * chips,
        (place, ids, weights, normed), flops=work + few,
    )
    incoming = [outgoing[0]] + [exchange(outgoing[m], 2 * m) for m in range(1, chips)]
    crossing = call(
        swap_kernel, jax.ShapeDtypeStruct((rows // 2, width + LANES), BF16), incoming,
        scalars=0,
    )
    crossed = exchange(crossing, 1)
    pick, label, mix_other = call(
        functools.partial(route_kernel, **sizes), plan,
        (place_other, ids_other, weights_other), flops=few,
    )
    outgoing_other = call(gather_kernel, sent, (pick, label, normed_other), scalars=0, flops=work)
    incoming_other = within(outgoing_other)
    experts = (expert_gate, expert_up, expert_down)
    kept, crossing = run_experts(
        incoming + [crossed], [cap] * chips + [rows // 2], [rows // 2] * 2, *experts
    )
    (results_other,) = run_experts([incoming_other], [rows], [rows], *experts)
    back_other = within(results_other)
    crossed = exchange(crossing, 1)
    piece = jax.ShapeDtypeStruct((2 * cap, width), BF16)
    results = call(merge_kernel, [piece] * chips, (kept, crossed), scalars=0)
    back = [results[0]] + [exchange(results[m], 2 * m) for m in range(1, chips)]

    block = shared_gate.shape[0]
    full = pltpu.VMEM((devices * block, cut), BF16)
    shape = jax.ShapeDtypeStruct((count, width), F32)
    shared_own, shared_other = call(
        functools.partial(shared_kernel, offsets=tuple(offsets)),
        (shape, shape),
        (me.reshape(1), parts, far_parts, normed, normed_other),
        flops=12 * count * width * cut,
        scratch_shapes=[full, full, full],
    )
    partial = call(
        combine_kernel, dense, (mix_other, back_other, shared_other),
        scalars=0, flops=2 * work,
    )
    from_other = exchange(partial, half)
    total = call(
        own_kernel, shape, (mix, shared_own, *back),
        scalars=0, flops=2 * work, scratch_shapes=[pltpu.VMEM((rows, width), BF16)],
    )
    return call(add_kernel, dense, (total, from_other), scalars=0, flops=count * width)


def shared_steps(devices):
    half = devices // 2
    bits = [1 << b for b in range(devices.bit_length() - 3, 0, -1)]
    return [half] + bits[1:] + [bits[0], 1]


def solution(mesh):
    return jax.shard_map(
        per_device,
        mesh=mesh,
        in_specs=(
            P("ep", None),
            P(),
            P("ep", None),
            P("ep", None),
            P("ep", None, None),
            P("ep", None, None),
            P("ep", None, None),
            P("ep", None),
            P("ep", None),
            P(None, "ep"),
        ),
        out_specs=P("ep", None),
        check_vma=False,
    )
```

```python
import functools

import jax
import jax.numpy as jnp
from jax import lax
from jax.experimental import pallas as pl
from jax.experimental.pallas import tpu as pltpu
from jax.sharding import PartitionSpec as P


EPS = 1e-06
LANES = 128
F32 = jnp.float32
BF16 = jnp.bfloat16


VMEM = pl.BlockSpec(memory_space=pltpu.VMEM)
SMEM = pl.BlockSpec(memory_space=pltpu.SMEM)


def routes(place_ref, ids_ref, weights_ref, local_experts, slots, cap):
    top, count = ids_ref.shape
    rows = slots * cap
    ids = ids_ref[...]
    weights = weights_ref[...]
    target = ids // local_experts
    local = (ids % local_experts).astype(F32)
    device = place_ref[0] + (
        lax.broadcasted_iota(jnp.int32, (slots, count), 0) ^ place_ref[1]
    )
    zero = jnp.zeros((slots, count), F32)
    member, weight, label = zero, zero, zero
    for k in range(top):
        hit = target[k : k + 1, :] == device
        member = jnp.where(hit, 1.0, member)
        weight = jnp.where(hit, weights[k : k + 1, :], weight)
        label = jnp.where(hit, local[k : k + 1, :], label)
    square = lambda dim: lax.broadcasted_iota(jnp.int32, (count, count), dim)
    before = (square(0) < square(1)).astype(BF16)
    rank = jnp.dot(member.astype(BF16), before, preferred_element_type=F32)
    rank = jnp.where(member > 0.0, rank, -1.0)
    row = lax.broadcasted_iota(jnp.int32, (rows, slots), 0)
    expand = (row // cap == lax.broadcasted_iota(jnp.int32, (rows, slots), 1)).astype(BF16)
    spread = lambda array: jnp.dot(expand, array.astype(BF16), preferred_element_type=F32)
    want = (lax.broadcasted_iota(jnp.int32, (rows, count), 0) % cap).astype(F32)
    pick = (spread(rank) == want).astype(F32)
    labels = jnp.sum(pick * spread(label), axis=1, keepdims=True)
    labels = jnp.broadcast_to(labels, (rows, LANES)).astype(BF16)
    high = weight.astype(BF16).astype(F32)
    mix = jnp.concatenate([(pick * spread(high)).T, (pick * spread(weight - high)).T], axis=0)
    return pick.astype(BF16), labels, mix.astype(BF16)


def norm_kernel(tokens_ref, gain_ref, out_ref):
    values = tokens_ref[...].astype(F32)
    scale = lax.rsqrt(jnp.mean(values * values, axis=-1, keepdims=True) + EPS)
    out_ref[...] = (values * scale * gain_ref[...]).astype(BF16)


def front_kernel(place_ref, ids_ref, weights_ref, x_ref, mix_ref, *out_refs, **sizes):
    pick, labels, mix = routes(place_ref, ids_ref, weights_ref, **sizes)
    mix_ref[...] = mix
    width = x_ref.shape[1]
    sent = jnp.dot(pick, x_ref[...], preferred_element_type=F32).astype(BF16)
    start = 0
    for out_ref in out_refs:
        stop = start + out_ref.shape[0]
        out_ref[:, :width] = sent[start:stop]
        out_ref[:, width:] = labels[start:stop]
        start = stop


def route_kernel(place_ref, ids_ref, weights_ref, pick_ref, label_ref, mix_ref, **sizes):
    pick_ref[...], label_ref[...], mix_ref[...] = routes(
        place_ref, ids_ref, weights_ref, **sizes
    )


def gather_kernel(pick_ref, label_ref, x_ref, out_ref):
    width = x_ref.shape[1]
    out_ref[:, :width] = jnp.dot(pick_ref[...], x_ref[...], preferred_element_type=F32).astype(
        BF16
    )
    out_ref[:, width:] = label_ref[...]


def join(refs, rows_ref, takes=None):
    start = 0
    for ref, take in zip(refs, takes or [ref.shape[0] for ref in refs]):
        rows_ref[start : start + take, :] = ref[:take]
        start += take


def swap_kernel(*refs):
    *in_refs, out_ref = refs
    cap = in_refs[0].shape[0] // 2
    for i, ref in enumerate(in_refs):
        out_ref[i * cap : (i + 1) * cap, :] = ref[cap:]


def merge_kernel(kept_ref, swapped_ref, *out_refs):
    cap = out_refs[0].shape[0] // 2
    for i, ref in enumerate(out_refs):
        ref[:cap] = kept_ref[i * cap : (i + 1) * cap, :]
        ref[cap:] = swapped_ref[i * cap : (i + 1) * cap, :]


def combined(mix_ref, back_ref):
    both = jnp.dot(mix_ref[...], back_ref[...], preferred_element_type=F32)
    count = both.shape[0] // 2
    return both[:count] + both[count:]


def combine_kernel(mix_ref, back_ref, shared_ref, out_ref):
    out_ref[...] = (combined(mix_ref, back_ref) + shared_ref[...]).astype(BF16)


def own_kernel(mix_ref, shared_ref, *refs):
    *back_refs, out_ref, rows_ref = refs
    join(back_refs, rows_ref)
    out_ref[...] = combined(mix_ref, rows_ref) + shared_ref[...]


def add_kernel(own_ref, other_ref, out_ref):
    out_ref[...] = (own_ref[...] + other_ref[...].astype(F32)).astype(BF16)


def expert_kernel(gate_ref, up_ref, down_ref, *refs, takes, results, cuts, outs):
    in_refs, out_refs = refs[: len(takes)], refs[len(takes) : len(takes) + results]
    gate_buf, up_buf, down_buf, hidden_ref, sems, *rest = refs[len(takes) + results :]
    rows_ref = rest[0] if rest else in_refs[0]
    experts, width, hidden = gate_ref.shape
    block = hidden // cuts
    parts = [(e, pl.ds(j * block, block)) for e in range(experts) for j in range(cuts)]
    firsts = []
    for i, (e, cols) in enumerate(parts):
        pair = [
            pltpu.make_async_copy(src.at[e, :, cols], dst.at[i], sems.at[k, i])
            for k, (src, dst) in enumerate(((gate_ref, gate_buf), (up_ref, up_buf)))
        ]
        for copy in pair:
            copy.start()
        firsts.append(pair)
    piece = width // outs
    seconds = []
    for i in range(outs):
        cols = pl.ds(i * piece, piece)
        copy = pltpu.make_async_copy(down_ref.at[:, cols], down_buf.at[i], sems.at[2, i])
        copy.start()
        seconds.append(copy)
    if rest:
        join(in_refs, rows_ref, takes)
    for i, (e, _) in enumerate(parts):
        for copy in firsts[i]:
            copy.wait()
        rows = rows_ref[:, :width]
        mine = rows_ref[:, width:][:, :1].astype(F32) == float(e)
        gate_val = jnp.dot(rows, gate_buf[i], preferred_element_type=F32)
        up_val = jnp.dot(rows, up_buf[i], preferred_element_type=F32)
        value = jnp.where(mine, gate_val / (1.0 + jnp.exp(-gate_val)) * up_val, 0.0)
        hidden_ref[:, i * block : (i + 1) * block] = value.astype(BF16)
    for i, copy in enumerate(seconds):
        copy.wait()
        result = jnp.dot(
            hidden_ref[...], down_buf[i], preferred_element_type=F32
        ).astype(BF16)
        start = 0
        for out_ref in out_refs:
            stop = start + out_ref.shape[0]
            out_ref[:, i * piece : (i + 1) * piece] = result[start:stop]
            start = stop


def run_experts(rows, takes, results, w_gate, w_up, w_down):
    experts, width, hidden = w_gate.shape
    cuts, outs = 2, 2
    steps = experts * cuts
    block, piece = hidden // cuts, width // outs
    count = sum(takes)
    scratch = [
        pltpu.VMEM((steps, width, block), BF16),
        pltpu.VMEM((steps, width, block), BF16),
        pltpu.VMEM((outs, experts * hidden, piece), BF16),
        pltpu.VMEM((count, experts * hidden), BF16),
        pltpu.SemaphoreType.DMA((3, max(steps, outs))),
    ]
    if len(rows) > 1:
        scratch.append(pltpu.VMEM((count, rows[0].shape[1]), BF16))
    return pl.pallas_call(
        functools.partial(
            expert_kernel, takes=tuple(takes), results=len(results), cuts=cuts, outs=outs
        ),
        in_specs=[pl.BlockSpec(memory_space=pltpu.HBM)] * 3 + [VMEM] * len(rows),
        out_specs=[VMEM] * len(results),
        out_shape=[jax.ShapeDtypeStruct((part, width), BF16) for part in results],
        scratch_shapes=scratch,
        cost_estimate=pl.CostEstimate(
            flops=6 * count * experts * width * hidden,
            bytes_accessed=6 * experts * width * hidden + 4 * count * width,
            transcendentals=count * experts * hidden,
        ),
        compiler_params=pltpu.CompilerParams(vmem_limit_bytes=60 << 20),
    )(w_gate, w_up, w_down.reshape(experts * hidden, width), *rows)


def shared_kernel(me_ref, *refs, offsets, hops):
    parts_refs = refs[: len(hops)]
    own_ref, other_ref, out_own_ref, out_other_ref, gate_ref, up_ref, down_ref = refs[len(hops) :]
    block = parts_refs[0].shape[2]
    for parts_ref, hop in zip(parts_refs, hops):
        me = me_ref[0] ^ hop
        for place, offset in enumerate(offsets):
            start = pl.multiple_of((me ^ offset) * block, block)
            gate_ref[pl.ds(start, block), :] = parts_ref[place, 0]
            up_ref[pl.ds(start, block), :] = parts_ref[place, 1]
            down_ref[pl.ds(start, block), :] = parts_ref[place, 2]
    for x_ref, out_ref in ((own_ref, out_own_ref), (other_ref, out_other_ref)):
        x = x_ref[...]
        gate_val = jnp.dot(x, gate_ref[...], preferred_element_type=F32)
        up_val = jnp.dot(x, up_ref[...], preferred_element_type=F32)
        hidden = (gate_val / (1.0 + jnp.exp(-gate_val)) * up_val).astype(BF16)
        out_ref[...] = lax.dot_general(
            hidden, down_ref[...], (((1,), (1,)), ((), ())), preferred_element_type=F32
        )


def call(kernel, out, args, scalars=1, flops=0, vmem=24, **options):
    shapes = jax.tree.leaves(out)
    specs = jax.tree.map(lambda _: VMEM, out)
    return pl.pallas_call(
        kernel,
        in_specs=[SMEM] * scalars + [VMEM] * (len(args) - scalars),
        out_specs=specs,
        out_shape=out,
        cost_estimate=pl.CostEstimate(
            flops=flops,
            bytes_accessed=sum(a.size * a.dtype.itemsize for a in list(args) + shapes),
            transcendentals=0,
        ),
        compiler_params=pltpu.CompilerParams(vmem_limit_bytes=vmem << 20),
        **options,
    )(*args)


def per_device(
    tokens,
    norm_gain,
    expert_ids,
    gate_weights,
    expert_gate,
    expert_up,
    expert_down,
    shared_gate,
    shared_up,
    shared_down,
):
    devices = lax.axis_size("ep")
    me = lax.axis_index("ep").astype(jnp.int32)
    half = devices // 2
    side = me // half
    count, top = expert_ids.shape
    width = tokens.shape[1]
    mean_rows = count * top // devices
    cap = -(-(mean_rows + mean_rows // 2) // 8) * 8
    rows = half * cap
    sizes = dict(local_experts=expert_gate.shape[0], slots=half, cap=cap)
    groups = [list(range(half)), list(range(half, devices))]

    def exchange(array, bit):
        return lax.ppermute(array, "ep", [(i, i ^ bit) for i in range(devices)])

    def within(array):
        return lax.all_to_all(array, "ep", 0, 0, axis_index_groups=groups, tiled=True)

    base = side * half
    place = jnp.stack([base, me % half])
    place_other = jnp.stack([base, jnp.zeros_like(me)])
    dense = jax.ShapeDtypeStruct((count, width), BF16)
    plan = (
        jax.ShapeDtypeStruct((rows, count), BF16),
        jax.ShapeDtypeStruct((rows, LANES), BF16),
        jax.ShapeDtypeStruct((2 * count, rows), BF16),
    )
    sent = jax.ShapeDtypeStruct((rows, width + LANES), BF16)
    work = 2 * rows * count * width
    few = 8 * rows * count * half

    parts = jnp.stack([shared_gate, shared_up, shared_down.T])[None]
    cut = parts.shape[3] // 2
    offsets = [0]
    *steps, last, _ = shared_steps(devices)
    for bit in steps:
        if bit == half:
            low, high = parts[..., :cut], parts[..., cut:]
            mine = jnp.where(side == 0, low, high)
            theirs = jnp.where(side == 0, high, low)
        else:
            mine = theirs = parts
        parts = jnp.concatenate([mine, exchange(theirs, bit)], axis=0)
        offsets += [offset ^ bit for offset in offsets]
    far = exchange(parts, last)
    shares = (parts, far, exchange(parts, 1), exchange(far, 1))

    ids, weights = expert_ids.T, gate_weights.T
    ids_other = exchange(ids, half)
    weights_other = exchange(weights, half)
    chips = half // 2
    piece = jax.ShapeDtypeStruct((2 * cap, width + LANES), BF16)
    normed = call(
        norm_kernel, dense, (tokens, norm_gain.reshape(1, width)),
        scalars=0, flops=8 * count * width,
    )
    normed_other = exchange(normed, half)
    mix, *outgoing = call(
        functools.partial(front_kernel, **sizes), [plan[2]] + [piece] * chips,
        (place, ids, weights, normed), flops=work + few,
    )
    incoming = [outgoing[0]] + [exchange(outgoing[m], 2 * m) for m in range(1, chips)]
    crossing = call(
        swap_kernel, jax.ShapeDtypeStruct((rows // 2, width + LANES), BF16), incoming,
        scalars=0,
    )
    crossed = exchange(crossing, 1)
    pick, label, mix_other = call(
        functools.partial(route_kernel, **sizes), plan,
        (place_other, ids_other, weights_other), flops=few,
    )
    outgoing_other = call(gather_kernel, sent, (pick, label, normed_other), scalars=0, flops=work)
    incoming_other = within(outgoing_other)
    experts = (expert_gate, expert_up, expert_down)
    kept, crossing = run_experts(
        incoming + [crossed], [cap] * chips + [rows // 2], [rows // 2] * 2, *experts
    )
    (results_other,) = run_experts([incoming_other], [rows], [rows], *experts)
    back_other = within(results_other)
    crossed = exchange(crossing, 1)
    piece = jax.ShapeDtypeStruct((2 * cap, width), BF16)
    results = call(merge_kernel, [piece] * chips, (kept, crossed), scalars=0)
    back = [results[0]] + [exchange(results[m], 2 * m) for m in range(1, chips)]

    block = shared_gate.shape[0]
    full = pltpu.VMEM((devices * block, cut), BF16)
    shape = jax.ShapeDtypeStruct((count, width), F32)
    shared_own, shared_other = call(
        functools.partial(
            shared_kernel, offsets=tuple(offsets), hops=(0, last, 1, last ^ 1)
        ),
        (shape, shape),
        (me.reshape(1), *shares, normed, normed_other),
        flops=12 * count * width * cut,
        scratch_shapes=[full, full, full],
    )
    partial = call(
        combine_kernel, dense, (mix_other, back_other, shared_other),
        scalars=0, flops=2 * work,
    )
    from_other = exchange(partial, half)
    total = call(
        own_kernel, shape, (mix, shared_own, *back),
        scalars=0, flops=2 * work, scratch_shapes=[pltpu.VMEM((rows, width), BF16)],
    )
    return call(add_kernel, dense, (total, from_other), scalars=0, flops=count * width)


def shared_steps(devices):
    half = devices // 2
    bits = [1 << b for b in range(devices.bit_length() - 3, 0, -1)]
    return [half] + bits[1:] + [bits[0], 1]


def solution(mesh):
    return jax.shard_map(
        per_device,
        mesh=mesh,
        in_specs=(
            P("ep", None),
            P(),
            P("ep", None),
            P("ep", None),
            P("ep", None, None),
            P("ep", None, None),
            P("ep", None, None),
            P("ep", None),
            P("ep", None),
            P(None, "ep"),
        ),
        out_specs=P("ep", None),
        check_vma=False,
    )
```
